32 devices in a mesh: grp: 2 (over y), sp: 16 (over z, x, core), tp: 1.
Axes of the slice: x: 2, y: 2, z: 4, core: 2. Of those that a mesh axis runs over, the one named last changes fastest.
Arguments:
- glu_value: bfloat16 [4096, 2048], P(('grp', 'sp'), 'tp'), parts along dimension 0, may hold values from -6 to 6
- glu_gate: bfloat16 [4096, 2048], P(('grp', 'sp'), 'tp'), parts along dimension 0, may hold values from -9 to 9
- segments: int32 [4096], P(('grp', 'sp')), parts along dimension 0, may hold values from 0 to 3, never falling along the last dimension, each value on 1 to 1024 neighbouring positions
- conv_kernel: float32 [31, 2048], P(None, 'tp'), may hold values from -3.5 to 3.5
- norm_gain: float32 [2048], P('tp'), may hold values from 0.1 to 1.9
- norm_bias: float32 [2048], P('tp'), may hold values from -3 to 3
- residual: bfloat16 [4096, 2048], P(('grp', 'sp'), 'tp'), parts along dimension 0, may hold values from -6 to 6
- out_weight: bfloat16 [2048, 2048], P('tp'), may hold values from -0.125 to 0.125
- rms_gain: float32 [2048], replicated, may hold values from 0.1 to 1.9
- experts: int32 [4096, 4], P(('grp', 'sp')), parts along dimension 0, may hold values from 0 to 15, all different within a row; in each aligned block of 128 rows (0 to 127, 128 to 255, ...) at most 64 rows name the same one
- route_weights: float32 [4096, 4], P(('grp', 'sp')), parts along dimension 0, may hold values from 0.1 to 1
- glu_weight: bfloat16 [16, 2048, 2048], P('sp', None, 'tp'), may hold values from -0.5 to 0.5
- lin_weight: bfloat16 [16, 2048, 2048], P('sp', None, 'tp'), may hold values from -0.5 to 0.5
- down_weight: bfloat16 [16, 2048, 2048], P('sp', None, 'tp'), may hold values from -0.015625 to 0.015625
Outputs:
- layer_output: bfloat16 [4096, 2048], P(('grp', 'sp'), 'tp'), parts along dimension 0
The draws below stay inside these ranges and needn't reach their ends.
There are 2 independent parts, one for each index of `grp`. The reference program is written for one: setup_inputs(seed, part) draws one part's arguments, and reference() takes and returns one part's arrays. A program takes and returns all parts, laid end to end along the dimension named above; an argument that names none is the same for every part. Nothing has to cross between parts.
Inputs may be any that keep to these rules, and one draw needn't show every extreme that they name: Each row names 4 different experts. In each aligned block of 128 rows no expert is named by more than 64 rows, and in some block an expert is named by exactly 64 rows. `segments`: never falling along positions; a document holds from 1 up to 1024 positions, and one holds exactly that many.
All inputs are finite; a program needn't handle non-finite values.
Results may differ from the reference program's by a relative error of at most 0.017.
Values may be sent and summed in bfloat16 or wider, within the bound.
A program may use at most 128 MiB of HBM per device.

```python
import math
import jax
import jax.numpy as jnp
import numpy as np
from jax import lax

D = 2048
FF = 2048
TAPS = 31
TOPK = 4
TOK_DEV = 128
TOKENS = 2048
EXPERTS = 16
CAP = 64
N_SP = 16
N_TP = 1


def draw_conv_kernel(key, part):
    channel = jnp.arange(D, dtype=jnp.float32) / D
    values = jnp.clip(jax.random.normal(key, (TAPS, D), jnp.float32), -4.0, 4.0)
    ramp = 3.0 ** channel
    return values * ramp[None, :] * TAPS ** (-0.5)


def level_of(key, shape, shards, least, largest):
    loudness, own = 1.0, jax.random.fold_in(key, 6)
    for position, shards_of in shards:
        heights = jnp.exp(jax.random.uniform(jax.random.fold_in(own, position), (shards_of,), jnp.float32, least / len(shards), largest / len(shards)))
        loudness = loudness * jnp.repeat(heights, shape[position] // shards_of).reshape([-1 if axis == position else 1 for axis in range(len(shape))])
    return loudness


def split_up(amount, total, most, lean):
    portions = [(1 << 20) // math.isqrt(standing ** lean) + 1 for standing in range(2, amount + 1)]
    surplus, holding = total - most - (amount - 1), [1] * (amount - 1)
    while surplus > 0:
        candidates = [i for i in range(amount - 1) if holding[i] < most]
        mass, budget = sum([portions[i] for i in candidates]), surplus
        for i in candidates:
            extra = min(most - holding[i], max(1, budget * portions[i] // mass), surplus)
            holding[i] = holding[i] + extra
            surplus = surplus - extra
    return np.array([most] + holding)


def uneven(stream_key, number_of, total, limit, skew):
    if number_of == 2:
        one = jax.random.randint(stream_key, (), max(1, total - limit), min(limit, total - 1) + 1)
        return jnp.stack([one, total - one])
    lengths = jnp.asarray(split_up(number_of, total, limit, skew), jnp.int32)
    twos = (number_of - 1) // 2
    source_of, taker = lengths[1:1 + 2 * twos:2], lengths[2:2 + 2 * twos:2]
    margin = jnp.minimum(source_of - 1, limit - taker)
    moved = jax.random.randint(jax.random.fold_in(stream_key, 1), (twos,), 0, 1 << 20) % (margin + 1)
    lengths = lengths.at[1:1 + 2 * twos:2].set(source_of - moved).at[2:2 + 2 * twos:2].set(taker + moved)
    return lengths[jax.random.permutation(jax.random.fold_in(stream_key, 2), number_of)]


def routed_block(key, own, number, rows, count, top, bound, skew):
    order = jax.random.permutation(key, count)
    crowded, ordinary = portions_of(count, rows * top, bound, skew, True), portions_of(count, rows * top, bound, skew, False)
    places = jnp.arange(count)

    def named(lengths, offset_by):
        used = int((lengths > 0).sum())
        fixed = max(1, used // 4)
        moved = fixed + (places - fixed + offset_by * (used - fixed)) % max(1, count - fixed)
        return jnp.zeros((count,), jnp.int32).at[order[jnp.where(places < fixed, places, moved)]].set(jnp.asarray(lengths, jnp.int32))

    lengths = jnp.where(number % 4 == 0, named(crowded, number // 4), named(ordinary, number - number // 4 - 1))
    mixed = jax.random.permutation(jax.random.fold_in(own, 3), count)
    source_of, taker = mixed[0:count // 2 * 2:2], mixed[1:count // 2 * 2:2]
    slack = jnp.minimum(lengths[source_of] - 1, bound - lengths[taker]) // 2
    slack = jnp.where((source_of == order[0]) | (taker == order[0]) | (lengths[taker] == 0), 0, jnp.maximum(slack, 0))
    moved = jax.random.randint(jax.random.fold_in(own, 4), (count // 2,), 0, 1 << 20) % (slack + 1)
    lengths = lengths.at[source_of].add(-moved).at[taker].add(moved)
    members = jnp.searchsorted(jnp.cumsum(lengths), jnp.arange(rows * top), side="right").astype(jnp.int32)
    table = members.reshape(top, rows).T
    table = table[jax.random.permutation(jax.random.fold_in(own, 1), rows)]
    offset_by = jax.random.randint(jax.random.fold_in(own, 2), (rows, 1), 0, top)
    return jnp.take_along_axis(table, (jnp.arange(top)[None, :] + offset_by) % top, axis=1)


def portions_of(number_of, total, bound, slope, full):
    portions = [(1 << 20) // math.isqrt(standing ** slope) + 1 for standing in range(1, number_of + 1)]
    largest = bound if full else min(bound, max(-(-total // number_of), total * portions[0] // sum(portions)))
    least = 1 if total - largest >= number_of - 1 else 0
    holding, surplus = [largest] + [least] * (number_of - 1), total - largest - least * (number_of - 1)
    while surplus > 0:
        candidates = [i for i in range(1, number_of) if holding[i] < largest] or [i for i in range(1, number_of) if holding[i] < bound]
        whole, remaining = sum([portions[i] for i in candidates]), surplus
        for i in candidates:
            more = min(bound - holding[i], max(1, remaining * portions[i] // whole), surplus)
            holding[i] = holding[i] + more
            surplus = surplus - more
    return np.array(holding)


def noise(rng, extent, scale, bound, split=(), held_as=jnp.bfloat16):
    loudness = level_of(rng, extent, split, -0.22, 0.18) if split else 1.0
    values = jax.random.normal(rng, extent, jnp.float32) * scale * loudness
    return jnp.minimum(jnp.maximum(values, -bound), bound).astype(held_as)


def setup_inputs(seed: int = 0, part: int = 0) -> dict:
    seeds = jax.random.split(jax.random.key(seed), 15)
    part_keys = jax.random.split(jax.random.fold_in(seeds[14], part), 15)
    glu_value = noise(part_keys[0], (TOKENS, D), 1.0, 6.0, ((0, 16),))
    glu_gate = noise(part_keys[1], (TOKENS, D), 1.5, 9.0, ((0, 16),))
    segments = jnp.searchsorted(jnp.cumsum(uneven(part_keys[2], max(2, N_SP // 4), TOKENS, TOKENS // 2, 1)), jnp.arange(TOKENS), side="right").astype(jnp.int32)
    conv_kernel = draw_conv_kernel(jax.random.fold_in(seeds[14], 71), part)
    norm_gain = jnp.clip(1.0 + 0.18 * jax.random.normal(seeds[4], (D,), jnp.float32), 0.1, 1.9)
    norm_bias = noise(seeds[5], (D,), 0.5, 3.0, (), jnp.float32)
    residual = noise(part_keys[6], (TOKENS, D), 1.0, 6.0, ((0, 16),))
    out_weight = noise(seeds[7], (D, D), D ** -0.5, 0.125)
    rms_gain = jnp.clip(1.0 + 0.18 * jax.random.normal(seeds[8], (D,), jnp.float32), 0.1, 1.9)
    experts_keys = jax.random.split(jax.random.fold_in(part_keys[9], 1), TOKENS // TOK_DEV)
    experts_turns = jax.random.permutation(jax.random.fold_in(part_keys[9], 3), TOKENS // TOK_DEV)
    experts = jax.vmap(lambda own, number: routed_block(jax.random.fold_in(part_keys[9], 2), own, number, TOK_DEV, EXPERTS, TOPK, CAP, 2))(experts_keys, experts_turns).reshape((TOKENS, TOPK))
    route_weights = jnp.clip(jnp.exp(math.log(1.0) - 2.3025851 * jax.random.uniform(part_keys[10], (TOKENS, TOPK), jnp.float32) ** level_of(part_keys[10], (TOKENS, TOPK), ((0, 16),), -0.2, 0.2)), 0.1, 1.0)
    glu_weight = noise(seeds[11], (EXPERTS, D, FF), (D // 16) ** -0.5, 0.5, ((0, 16),))
    lin_weight = noise(seeds[12], (EXPERTS, D, FF), (D // 16) ** -0.5, 0.5, ((0, 16),))
    down_weight = noise(seeds[13], (EXPERTS, FF, D), (FF * 64) ** -0.5, 0.015625, ((0, 16),))
    return dict(glu_value=glu_value, glu_gate=glu_gate, segments=segments, conv_kernel=conv_kernel, norm_gain=norm_gain, norm_bias=norm_bias, residual=residual, out_weight=out_weight, rms_gain=rms_gain, experts=experts, route_weights=route_weights, glu_weight=glu_weight, lin_weight=lin_weight, down_weight=down_weight)


EPSILON = 1e-05
CLAMP_LIMIT = 7.0
SIGMOID_SCALE = 1.702

def clamped_unit(gate_pre, lin_pre):
    gate_clip = jnp.minimum(gate_pre, CLAMP_LIMIT)
    linear = jnp.clip(lin_pre, -CLAMP_LIMIT, CLAMP_LIMIT)
    return gate_clip * jax.nn.sigmoid(SIGMOID_SCALE * gate_clip) * (linear + 1.0)

def reference(glu_value, glu_gate, segments, conv_kernel, norm_gain, norm_bias, residual, out_weight, rms_gain, experts, route_weights, glu_weight, lin_weight, down_weight):
    glu_out = (glu_value.astype(jnp.float32) * jax.nn.sigmoid(glu_gate.astype(jnp.float32))).astype(jnp.bfloat16)
    glu_float = glu_out.astype(jnp.float32)
    conv_sum = jnp.zeros((TOKENS, D), jnp.float32)
    for offset in range(TAPS):
        shifted = jnp.pad(glu_float, ((offset, 0), (0, 0)))[:TOKENS]
        shifted_segments = jnp.pad(segments, (offset, 0), constant_values=-1)[:TOKENS]
        same_document = (shifted_segments == segments).astype(jnp.float32)
        conv_sum = conv_sum + conv_kernel[offset][None, :] * shifted * same_document[:, None]
    row_mean = lax.optimization_barrier(jnp.sum(conv_sum, axis=1, keepdims=True)) / D
    row_var = lax.optimization_barrier(jnp.sum(conv_sum * conv_sum, axis=1, keepdims=True)) / D - row_mean * row_mean
    normed_conv = (conv_sum - row_mean) * lax.rsqrt(row_var + EPSILON) * norm_gain + norm_bias
    swished = jax.nn.silu(normed_conv).astype(jnp.bfloat16)
    local_width = D // N_TP
    conv_out = jnp.zeros((TOKENS, D), jnp.float32)
    for piece_index in range(N_TP):
        lower = piece_index * local_width
        partial_value = jnp.dot(swished[:, lower:lower + local_width], out_weight[lower:lower + local_width], preferred_element_type=jnp.float32)
        conv_out = conv_out + partial_value.astype(jnp.bfloat16).astype(jnp.float32)
    updated = (residual.astype(jnp.float32) + conv_out).astype(jnp.bfloat16)
    updated_float = updated.astype(jnp.float32)
    normed = (updated_float * lax.rsqrt(lax.optimization_barrier(jnp.mean(updated_float * updated_float, axis=1, keepdims=True)) + EPSILON) * rms_gain).astype(jnp.bfloat16)
    normed_pad = jnp.concatenate([normed, jnp.zeros((1, D), jnp.bfloat16)], axis=0)
    flat_experts = experts.reshape(-1)
    flat_weights = jnp.concatenate([route_weights.reshape(-1), jnp.zeros((1,), jnp.float32)])
    slot_rows = N_SP * CAP

    def expert_step(accum_sum, inputs):
        glu_matrix, lin_matrix, down_matrix, expert_id = inputs
        chosen = jnp.nonzero(flat_experts == expert_id, size=slot_rows, fill_value=TOKENS * TOPK)[0].astype(jnp.int32)
        token_ids = (chosen // TOPK).astype(jnp.int32)
        gathered = normed_pad[token_ids]
        gate_pre = jnp.dot(gathered, glu_matrix, preferred_element_type=jnp.float32)
        lin_pre = jnp.dot(gathered, lin_matrix, preferred_element_type=jnp.float32)
        hidden = clamped_unit(gate_pre, lin_pre).astype(jnp.bfloat16)
        result = jnp.dot(hidden, down_matrix, preferred_element_type=jnp.float32).astype(jnp.bfloat16)
        weighted = result.astype(jnp.float32) * flat_weights[chosen][:, None]
        return (accum_sum.at[token_ids].add(weighted), None)
    accum_sum, unused = lax.scan(expert_step, jnp.zeros((TOKENS + 1, D), jnp.float32), (glu_weight, lin_weight, down_weight, jnp.arange(EXPERTS, dtype=jnp.int32)))
    return (updated_float + accum_sum[:TOKENS]).astype(jnp.bfloat16)
```

```python
import functools
import jax
import jax.numpy as jnp
from jax import lax
from jax.experimental import pallas as pl
from jax.experimental.pallas import tpu as pltpu
from jax.sharding import PartitionSpec as P

EPSILON = 1e-05
CLAMP_LIMIT = 7.0
SIGMOID_SCALE = 1.702


def passed_along(array, axis, by):
    length = lax.axis_size(axis)
    pairs = [(i, i + by) for i in range(length) if 0 <= i + by < length]
    return lax.ppermute(array, axis, pairs)


def clamped_unit(gate_pre, lin_pre):
    gate_clip = jnp.minimum(gate_pre, CLAMP_LIMIT)
    linear = jnp.clip(lin_pre, -CLAMP_LIMIT, CLAMP_LIMIT)
    return gate_clip * jax.nn.sigmoid(SIGMOID_SCALE * gate_clip) * (linear + 1.0)


def at_place(place, chips, inner):
    if inner == 1:
        return place
    depth = chips // 2
    column = place // depth
    return (place * (1 - column) + (chips - 1 - place) * column) * 2 + column


def place_of(chip, chips, inner):
    if inner == 1:
        return chip
    column = chip % 2
    depth = chip // 2
    return depth * (1 - column) + (chips - 1 - depth) * column


def remote(source, target, send_sem, recv_sem, device):
    return pltpu.make_async_remote_copy(
        src_ref=source,
        dst_ref=target,
        send_sem=send_sem,
        recv_sem=recv_sem,
        device_id={"sp": device},
        device_id_type=pl.DeviceIdType.MESH,
    )


def ring(sp_count, inner):
    chips = sp_count // 2
    me = lax.axis_index("sp")
    core = me % 2
    place = place_of(me // 2, chips, inner)

    def device_at(by, which=0):
        other = (core + which) % 2
        return at_place((place + by + chips) % chips, chips, inner) * 2 + other

    return chips, me, core, device_at


def gather_kernel(
    sp_count, inner, capacity, rows_ref, meta_ref, arrived_ref, rank_ref, weight_ref,
    gathered, all_meta, near_send, cw_send, ccw_send, row_recv, meta_send, meta_recv,
):
    chips, me, core, device_at = ring(sp_count, inner)
    partner = device_at(0, 1)
    tok_count = rows_ref.shape[0]
    half_rows = tok_count // 2
    far = chips // 2

    barrier = pltpu.get_barrier_semaphore()
    for by in range(1, sp_count):
        pl.semaphore_signal(
            barrier, inc=1, device_id={"sp": (me + by) % sp_count},
            device_id_type=pl.DeviceIdType.MESH,
        )
    pl.semaphore_wait(barrier, sp_count - 1)

    sent = []

    def start(source, owner, half, send_sem, device):
        copy = remote(
            source, gathered.at[owner, half], send_sem, row_recv.at[owner, half], device
        )
        copy.start()
        sent.append(copy)

    def landed(owner, half):
        remote(
            gathered.at[owner, half], gathered.at[owner, half],
            near_send.at[0, 0], row_recv.at[owner, half], partner,
        ).wait_recv()

    def own(half):
        return rows_ref.at[pl.ds(half * half_rows, half_rows)]

    for half in range(2):
        start(own(half), me, half, cw_send.at[0, half], device_at(1))
        start(own(half), me, half, ccw_send.at[0, half], device_at(-1))
    for by in range(1, sp_count):
        copy = remote(
            meta_ref, all_meta.at[me], meta_send.at[by], meta_recv.at[me],
            (me + by) % sp_count,
        )
        copy.start()
        sent.append(copy)
    for half in range(2):
        start(own(half), me, half, near_send.at[me, half], partner)
    all_meta[me] = meta_ref[...]
    for by in range(1, sp_count):
        owner = (me + by) % sp_count
        remote(
            all_meta.at[owner], all_meta.at[owner], meta_send.at[0], meta_recv.at[owner], partner
        ).wait_recv()

    mine = me.astype(jnp.float32)
    top_count = 4 if meta_ref.shape[0] == 8 else meta_ref.shape[0] // 2
    named = jnp.zeros((sp_count, tok_count), jnp.float32)
    weight = jnp.zeros((sp_count, tok_count), jnp.float32)
    for k in range(top_count):
        hit = (all_meta[:, k, :] == mine).astype(jnp.float32)
        named = named + hit
        weight = weight + hit * all_meta[:, top_count + k, :]
    upper = (
        lax.broadcasted_iota(jnp.int32, (tok_count, tok_count), 0)
        <= lax.broadcasted_iota(jnp.int32, (tok_count, tok_count), 1)
    ).astype(jnp.bfloat16)
    rank_ref[...] = named * jnp.dot(
        named.astype(jnp.bfloat16), upper, preferred_element_type=jnp.float32
    )
    weight_ref[...] = weight
    slots = lax.broadcasted_iota(jnp.int32, (capacity, tok_count), 0).astype(jnp.float32) + 1.0

    def dispatch(owner, lower, upper_rows):
        chosen = (rank_ref[pl.ds(owner, 1), :] == slots).astype(jnp.bfloat16)
        total = jnp.dot(
            chosen[:, :half_rows], lower, preferred_element_type=jnp.float32
        ) + jnp.dot(chosen[:, half_rows:], upper_rows, preferred_element_type=jnp.float32)
        arrived_ref[owner] = total.astype(jnp.bfloat16)

    def dispatch_gathered(owner):
        dispatch(owner, gathered[owner, 0], gathered[owner, 1])

    def dispatch_partner(by):
        owner = device_at(by, 1)
        for half in range(2):
            landed(owner, half)
        dispatch_gathered(owner)

    dispatch(me, rows_ref[:half_rows], rows_ref[half_rows:])
    dispatch_partner(0)
    for step in range(1, far + 1):
        for half in range(2):
            for way, sems in ((1, cw_send), (-1, ccw_send)):
                if step == far and half != (0 if way == 1 else 1):
                    continue
                owner = device_at(-way * step)
                landed(owner, half)
                block = gathered.at[owner, half]
                if step + 1 < far or (step + 1 == far and half == (0 if way == 1 else 1)):
                    start(block, owner, half, sems.at[step, half], device_at(way))
                start(block, owner, half, near_send.at[owner, half], partner)
        dispatch_gathered(device_at(step))
        if step < far:
            dispatch_gathered(device_at(-step))
        if step > 1:
            dispatch_partner(step - 1)
            dispatch_partner(1 - step)
    dispatch_partner(far)
    for copy in sent:
        copy.wait_send()


def gather_rows(rows, meta, sp_count, inner, capacity):
    tok_count, width = rows.shape
    far = sp_count // 4
    vmem = pl.BlockSpec(memory_space=pltpu.VMEM)
    sems = pltpu.SemaphoreType.DMA
    return pl.pallas_call(
        functools.partial(gather_kernel, sp_count, inner, capacity),
        out_shape=(
            jax.ShapeDtypeStruct((sp_count, capacity, width), jnp.bfloat16),
            jax.ShapeDtypeStruct((sp_count, tok_count), jnp.float32),
            jax.ShapeDtypeStruct((sp_count, tok_count), jnp.float32),
        ),
        in_specs=[vmem, vmem],
        out_specs=(vmem, vmem, vmem),
        scratch_shapes=[
            pltpu.VMEM((sp_count, 2, tok_count // 2, width), jnp.bfloat16),
            pltpu.VMEM((sp_count,) + meta.shape, jnp.float32),
            sems((sp_count, 2)),
            sems((far, 2)),
            sems((far, 2)),
            sems((sp_count, 2)),
            sems((sp_count,)),
            sems((sp_count,)),
        ],
        compiler_params=pltpu.CompilerParams(
            collective_id=1, has_side_effects=True, vmem_limit_bytes=48 * 1024 * 1024
        ),
    )(rows, meta)


def scatter_kernel(
    sp_count, inner, results_ref, rank_ref, weight_ref, updated_ref, out_ref,
    near_out, near_in, ring_out, ring_in, near_send, near_recv, ring_send, ring_recv,
):
    chips, me, core, device_at = ring(sp_count, inner)
    partner = device_at(0, 1)
    capacity = results_ref.shape[1]
    tok_count, width = updated_ref.shape
    part = width // 2
    far = chips // 2

    barrier = pltpu.get_barrier_semaphore()
    for device in (partner, device_at(1), device_at(-1)):
        pl.semaphore_signal(
            barrier, inc=1, device_id={"sp": device}, device_id_type=pl.DeviceIdType.MESH
        )
    pl.semaphore_wait(barrier, 3)

    slots = lax.broadcasted_iota(jnp.int32, (tok_count, capacity), 1).astype(jnp.float32) + 1.0

    def combined(owner, half):
        chosen = (rank_ref[owner] == slots).astype(jnp.bfloat16)
        return weight_ref[owner] * jnp.dot(
            chosen,
            results_ref[owner, :, half * part : (half + 1) * part],
            preferred_element_type=jnp.float32,
        )

    def near_copy(slot, half):
        return remote(
            near_out.at[slot, half], near_in.at[slot, half],
            near_send.at[slot, half], near_recv.at[slot, half], partner,
        )

    def ring_copy(way, number):
        return remote(
            ring_out.at[way, number], ring_in.at[way, number],
            ring_send.at[way, number], ring_recv.at[way, number],
            device_at(1 if way == 0 else -1),
        )

    def give(by, half):
        slot = by % chips
        near_out[slot, half] = combined(device_at(by, 1), half).astype(jnp.bfloat16)
        near_copy(slot, half).start()

    def own_sum(by, half):
        slot = by % chips
        mine = combined(device_at(by), half)
        near_copy(slot, half).wait_recv()
        return mine + near_in[slot, half].astype(jnp.float32)

    plan = [(far, 0), (far - 1, 1)]
    while plan[-2][0] > 1 or plan[-1][0] > 1:
        distance, half = plan[-2]
        plan.append((distance - 1, half))
        if len(plan) > 4 * far:
            break
    plan = [(distance, half) for distance, half in plan if distance >= 1]

    for distance, half in plan:
        give(distance, half)
        give(-distance, 1 - half)
    give(0, 0)
    give(0, 1)
    for number, (distance, half) in enumerate(plan):
        for way in range(2):
            by = distance if way == 0 else -distance
            column_half = half if way == 0 else 1 - half
            total = own_sum(by, column_half)
            if number >= 2:
                ring_copy(way, number - 2).wait_recv()
                total = total + ring_in[way, number - 2].astype(jnp.float32)
            ring_out[way, number] = total.astype(jnp.bfloat16)
            ring_copy(way, number).start()
    finals = len(plan)
    totals = [own_sum(0, 0), own_sum(0, 1)]
    for number in (finals - 2, finals - 1):
        half = plan[number][1]
        for way in range(2):
            ring_copy(way, number).wait_recv()
            column_half = half if way == 0 else 1 - half
            totals[column_half] = totals[column_half] + ring_in[way, number].astype(jnp.float32)
    for half in range(2):
        columns = slice(half * part, (half + 1) * part)
        out_ref[:, columns] = (
            updated_ref[:, columns].astype(jnp.float32) + totals[half]
        ).astype(jnp.bfloat16)
    for slot in range(chips):
        for half in range(2):
            near_copy(slot, half).wait_send()
    for number in range(finals):
        for way in range(2):
            ring_copy(way, number).wait_send()


def scatter_sums(results, rank, weight, updated, sp_count, inner):
    tok_count, width = updated.shape
    chips = sp_count // 2
    messages = chips - 1
    vmem = pl.BlockSpec(memory_space=pltpu.VMEM)
    sems = pltpu.SemaphoreType.DMA
    part = width // 2
    return pl.pallas_call(
        functools.partial(scatter_kernel, sp_count, inner),
        out_shape=jax.ShapeDtypeStruct((tok_count, width), jnp.bfloat16),
        in_specs=[vmem] * 4,
        out_specs=vmem,
        scratch_shapes=[
            pltpu.VMEM((chips, 2, tok_count, part), jnp.bfloat16),
            pltpu.VMEM((chips, 2, tok_count, part), jnp.bfloat16),
            pltpu.VMEM((2, messages, tok_count, part), jnp.bfloat16),
            pltpu.VMEM((2, messages, tok_count, part), jnp.bfloat16),
            sems((chips, 2)),
            sems((chips, 2)),
            sems((2, messages)),
            sems((2, messages)),
        ],
        compiler_params=pltpu.CompilerParams(
            collective_id=2, has_side_effects=True, vmem_limit_bytes=48 * 1024 * 1024
        ),
    )(results, rank, weight, updated)


def shards(
    inner,
    glu_value,
    glu_gate,
    segments,
    conv_kernel,
    norm_gain,
    norm_bias,
    residual,
    out_weight,
    rms_gain,
    experts,
    route_weights,
    glu_weight,
    lin_weight,
    down_weight,
):
    tok_count = glu_value.shape[0]
    local_width = glu_value.shape[1]
    model_width = out_weight.shape[1]
    kernel_reach = conv_kernel.shape[0] - 1
    top_count = experts.shape[1]
    local_experts = glu_weight.shape[0]
    sp_count = lax.axis_size("sp")
    expert_total = local_experts * sp_count
    capacity = min(tok_count, 2 * tok_count * top_count // expert_total)
    meta = jnp.concatenate([experts.astype(jnp.float32).T, route_weights.T], axis=0)
    glu_out = (glu_value.astype(jnp.float32) * jax.nn.sigmoid(glu_gate.astype(jnp.float32))).astype(
        jnp.bfloat16
    )
    tail_segments = segments[tok_count - kernel_reach :].astype(jnp.bfloat16) + 1
    tail = jnp.concatenate(
        [
            glu_out[tok_count - kernel_reach :],
            jnp.pad(tail_segments, (0, local_width - kernel_reach))[None],
        ],
        axis=0,
    )
    previous = passed_along(tail, "sp", 1)
    prev_rows = previous[:kernel_reach]
    prev_segments = previous[kernel_reach, :kernel_reach].astype(jnp.int32) - 1
    padded = jnp.concatenate([prev_rows, glu_out], axis=0).astype(jnp.float32)
    padded_segments = jnp.concatenate([prev_segments, segments], axis=0)
    conv_sum = jnp.zeros((tok_count, local_width), jnp.float32)
    for offset in range(kernel_reach + 1):
        lower = kernel_reach - offset
        window_rows = padded[lower : lower + tok_count]
        same_document = (padded_segments[lower : lower + tok_count] == segments).astype(jnp.float32)
        conv_sum = conv_sum + conv_kernel[offset][None, :] * window_rows * same_document[:, None]
    row_total, row_square = lax.psum(
        (jnp.sum(conv_sum, axis=1), jnp.sum(conv_sum * conv_sum, axis=1)), "tp"
    )
    row_mean = row_total / model_width
    row_var = row_square / model_width - row_mean * row_mean
    normed_conv = (conv_sum - row_mean[:, None]) * lax.rsqrt(row_var + EPSILON)[
        :, None
    ] * norm_gain + norm_bias
    swished = jax.nn.silu(normed_conv).astype(jnp.bfloat16)
    projected = jnp.dot(swished, out_weight, preferred_element_type=jnp.float32)
    conv_out = lax.psum_scatter(
        projected.astype(jnp.bfloat16), "tp", scatter_dimension=1, tiled=True
    ).astype(jnp.float32)
    updated = (residual.astype(jnp.float32) + conv_out).astype(jnp.bfloat16)
    updated_float = updated.astype(jnp.float32)
    whole_rows = lax.all_gather(updated, "tp", axis=1, tiled=True)
    whole_float = whole_rows.astype(jnp.float32)
    normed = (
        whole_float
        * lax.rsqrt(jnp.mean(whole_float * whole_float, axis=1, keepdims=True) + EPSILON)
        * rms_gain
    ).astype(jnp.bfloat16)
    arrived, rank, weight = gather_rows(normed, meta, sp_count, inner, capacity)
    arrived = arrived[:, None]
    gate_pre = jnp.einsum("slmd,ldf->slmf", arrived, glu_weight, preferred_element_type=jnp.float32)
    lin_pre = jnp.einsum("slmd,ldf->slmf", arrived, lin_weight, preferred_element_type=jnp.float32)
    hidden = clamped_unit(gate_pre, lin_pre).astype(jnp.bfloat16)
    summed = jnp.einsum(
        "slmf,lfd->slmd",
        lax.all_gather(hidden, "tp", axis=3, tiled=True),
        down_weight,
        preferred_element_type=jnp.float32,
    )
    results = summed[:, 0].astype(jnp.bfloat16)
    return scatter_sums(results, rank[:, :, None], weight[:, :, None], updated, sp_count, inner)


def solution(mesh):
    in_specs = (
        P(("grp", "sp"), "tp"),
        P(("grp", "sp"), "tp"),
        P(("grp", "sp")),
        P(None, "tp"),
        P("tp"),
        P("tp"),
        P(("grp", "sp"), "tp"),
        P("tp", None),
        P(),
        P(("grp", "sp"), None),
        P(("grp", "sp"), None),
        P("sp", None, "tp"),
        P("sp", None, "tp"),
        P("sp", None, "tp"),
    )
    out_specs = P(("grp", "sp"), "tp")
    coords = [getattr(d, "coords", (0, 0, 0)) for d in mesh.devices[0, :, 0]]
    inner = len({c[0] for c in coords})
    body = functools.partial(shards, inner)
    return jax.shard_map(body, mesh=mesh, in_specs=in_specs, out_specs=out_specs, check_vma=False)
```
